32 devices in a mesh: sp: 8 (over z, core), tp: 4 (over y, x).
Axes of the slice: x: 2, y: 2, z: 4, core: 2. Of those that a mesh axis runs over, the one named last changes fastest.
Arguments:
- cell_query_heads: bfloat16 [1024, 2048], P('sp', 'tp'), may hold values from -6 to 6
- cell_key_heads: bfloat16 [1024, 2048], P('sp', 'tp'), may hold values from -6 to 6
- cell_value_heads: bfloat16 [1024, 2048], P('sp', 'tp'), may hold values from -6 to 6
- output_gate_logits: bfloat16 [1024, 2048], P('sp', 'tp'), may hold values from -6 to 6
- input_gate_log: float32 [1024, 16], P('sp', 'tp'), may hold values from -7 to 310
- forget_gate_logits: float32 [1024, 16], P('sp', 'tp'), may hold values from 1 to 14
- extra_log_decay: float32 [1024, 16], P('sp', 'tp'), may hold values from -1 to 0
- documents: int32 [1024], P('sp'), may hold values from 0 to 7, never falling along the last dimension, each value on 1 to 256 neighbouring positions
- head_norm_gain: float32 [2048], P('tp'), may hold values from 0.1 to 1.9
- stream: bfloat16 [1024, 4096], P('sp', 'tp'), may hold values from -6 to 6
- output_weight: bfloat16 [2048, 4096], P(None, 'tp'), may hold values from -0.125 to 0.125
- expert_norm_gain: bfloat16 [4096], P('tp'), may hold values from 0.099609375 to 1.8984375
- expert_choice_index: int32 [1024, 2], P('sp'), may hold values from 0 to 7, all different within a row; in each aligned block of 128 rows (0 to 127, 128 to 255, ...) at most 64 rows name the same one
- routing_weight: float32 [1024, 2], P('sp'), may hold values from 0.2 to 1
- gate_weight: bfloat16 [8, 4096, 2048], P('sp', None, 'tp'), may hold values from -0.09375 to 0.09375
- up_weight: bfloat16 [8, 4096, 2048], P('sp', None, 'tp'), may hold values from -0.09375 to 0.09375
- down_weight: bfloat16 [8, 2048, 4096], P('sp', None, 'tp'), may hold values from -0.125 to 0.125
Outputs:
- output: bfloat16 [1024, 4096], P('sp', 'tp')
The draws below stay inside these ranges and needn't reach their ends.
Inputs may be any that keep to these rules, and one draw needn't show every extreme that they name: `expert_choice_index`: in the rows of one index of sp no expert is named more than 64 times, a bound that some block reaches. `documents`: never falling; each document 1 to 256 positions, one exactly 256.
All inputs are finite; a program needn't handle non-finite values.
Results may differ from the reference program's by a relative error of at most 0.01.
Values may be sent and summed in bfloat16 or wider, within the bound.
No kernel may reach another device: no remote copies, remote signals or barrier semaphores. Data moves between devices by JAX's collectives and lax.ppermute only.
A program may use at most 64 MiB of HBM per device.

```python
import math
import jax
import jax.numpy as jnp
import numpy as np
from jax import lax

D = 4096
CELL_HEADS = 16
HD = 128
FF = 2048
TOPK = 2
TOKENS_PER_SHARD = 128
DOCS = 8
SEQ = 1024
EXPERTS = 8
CAP = 64
DOC_MOST = 256
N_SP = 8


def draw_forget_gate_logits(key, part):
    head_key = jax.random.fold_in(key, 11)
    block_key = jax.random.fold_in(key, 12)
    noise_key = jax.random.fold_in(key, 13)
    fast_heads = jax.random.randint(head_key, (CELL_HEADS,), 0, 2) == 0
    level = jnp.where(fast_heads, jnp.log(40.0), jnp.log(SEQ / 1.5)).astype(jnp.float32)
    block_list = SEQ // TOKENS_PER_SHARD
    shift = jax.random.uniform(block_key, (block_list, 1, CELL_HEADS), jnp.float32, -0.7, 0.7)
    noise = 0.5 * jnp.clip(jax.random.normal(noise_key, (block_list, TOKENS_PER_SHARD, CELL_HEADS), jnp.float32), -3.0, 3.0)
    return (level[None, None, :] + shift + noise).reshape(SEQ, CELL_HEADS)


def draw_input_gate_log(key, part):
    base_key = jax.random.fold_in(key, 21)
    values = jnp.clip(jax.random.normal(base_key, (SEQ, CELL_HEADS), jnp.float32), -6.0, 6.0)
    return values


def draw_extra_log_decay(key, part):
    mark_key = jax.random.fold_in(key, 31)
    depth_key = jax.random.fold_in(key, 32)
    marks = jax.random.randint(mark_key, (SEQ, CELL_HEADS), 0, SEQ // 8) == 0
    depth = jax.random.uniform(depth_key, (SEQ, CELL_HEADS), jnp.float32, jnp.log(0.5), jnp.log(0.8))
    return jnp.where(marks, depth, 0.0).astype(jnp.float32)


def shard_levels(key, dims, pieces, smallest, high):
    level, own = 1.0, jax.random.fold_in(key, 6)
    for axis_at, parts in pieces:
        draws = jnp.exp(jax.random.uniform(jax.random.fold_in(own, axis_at), (parts,), jnp.float32, smallest / len(pieces), high / len(pieces)))
        level = level * jnp.repeat(draws, dims[axis_at] // parts).reshape([-1 if axis == axis_at else 1 for axis in range(len(dims))])
    return level


def length_profile(count, total, reach, slope):
    portions = [(1 << 20) // math.isqrt(rank ** slope) + 1 for rank in range(2, count + 1)]
    surplus, given = total - reach - (count - 1), [1] * (count - 1)
    while surplus > 0:
        free = [i for i in range(count - 1) if given[i] < reach]
        pool, left = sum([portions[i] for i in free]), surplus
        for i in free:
            extra = min(reach - given[i], max(1, left * portions[i] // pool), surplus)
            given[i] = given[i] + extra
            surplus = surplus - extra
    return np.array([reach] + given)


def ragged(own_key, number_of, total, limit, skew):
    if number_of == 2:
        one = jax.random.randint(own_key, (), max(1, total - limit), min(limit, total - 1) + 1)
        return jnp.stack([one, total - one])
    lengths = jnp.asarray(length_profile(number_of, total, limit, skew), jnp.int32)
    pairs = (number_of - 1) // 2
    giver, taker = lengths[1:1 + 2 * pairs:2], lengths[2:2 + 2 * pairs:2]
    margin = jnp.minimum(giver - 1, limit - taker)
    passed = jax.random.randint(jax.random.fold_in(own_key, 1), (pairs,), 0, 1 << 20) % (margin + 1)
    lengths = lengths.at[1:1 + 2 * pairs:2].set(giver - passed).at[2:2 + 2 * pairs:2].set(taker + passed)
    return lengths[jax.random.permutation(jax.random.fold_in(own_key, 2), number_of)]


def assign_block(stream_key, own, number, rows, number_of, top, most, lean):
    sequence = jax.random.permutation(stream_key, number_of)
    heavy_load, common = portions_of(number_of, rows * top, most, lean, True), portions_of(number_of, rows * top, most, lean, False)
    places = jnp.arange(number_of)

    def named(tallies, rotation):
        used = int((tallies > 0).sum())
        fixed = max(1, used // 4)
        moved = fixed + (places - fixed + rotation * (used - fixed)) % max(1, number_of - fixed)
        return jnp.zeros((number_of,), jnp.int32).at[sequence[jnp.where(places < fixed, places, moved)]].set(jnp.asarray(tallies, jnp.int32))

    tallies = jnp.where(number % 4 == 0, named(heavy_load, number // 4), named(common, number - number // 4 - 1))
    mixed = jax.random.permutation(jax.random.fold_in(own, 3), number_of)
    source_of, taker = mixed[0:number_of // 2 * 2:2], mixed[1:number_of // 2 * 2:2]
    room = jnp.minimum(tallies[source_of] - 1, most - tallies[taker]) // 2
    room = jnp.where((source_of == sequence[0]) | (taker == sequence[0]) | (tallies[taker] == 0), 0, jnp.maximum(room, 0))
    moved = jax.random.randint(jax.random.fold_in(own, 4), (number_of // 2,), 0, 1 << 20) % (room + 1)
    tallies = tallies.at[source_of].add(-moved).at[taker].add(moved)
    items = jnp.searchsorted(jnp.cumsum(tallies), jnp.arange(rows * top), side="right").astype(jnp.int32)
    table = items.reshape(top, rows).T
    table = table[jax.random.permutation(jax.random.fold_in(own, 1), rows)]
    rotation = jax.random.randint(jax.random.fold_in(own, 2), (rows, 1), 0, top)
    return jnp.take_along_axis(table, (jnp.arange(top)[None, :] + rotation) % top, axis=1)


def portions_of(number_of, total, most, skew, full):
    portions = [(1 << 20) // math.isqrt(rank ** skew) + 1 for rank in range(1, number_of + 1)]
    largest = most if full else min(most, max(-(-total // number_of), total * portions[0] // sum(portions)))
    least = 1 if total - largest >= number_of - 1 else 0
    given, rest = [largest] + [least] * (number_of - 1), total - largest - least * (number_of - 1)
    while rest > 0:
        free = [i for i in range(1, number_of) if given[i] < largest] or [i for i in range(1, number_of) if given[i] < most]
        pool, budget = sum([portions[i] for i in free]), rest
        for i in free:
            addition = min(most - given[i], max(1, budget * portions[i] // pool), rest)
            given[i] = given[i] + addition
            rest = rest - addition
    return np.array(given)


def centred(key, dims, scale, limit, split=(), held_as=jnp.bfloat16):
    drawn = jax.random.normal(key, dims, jnp.float32) * scale
    if len(split) > 0:
        drawn = shard_levels(key, dims, split, -0.22, 0.18) * drawn
    return jnp.clip(drawn, min=-limit, max=limit).astype(held_as)


def setup_inputs(seed: int = 0) -> dict:
    arg_keys = jax.random.split(jax.random.key(seed), 18)
    cell_query_heads = centred(arg_keys[0], (SEQ, CELL_HEADS * HD), 1.0, 6.0, ((0, 8), (1, 4)))
    cell_key_heads = centred(arg_keys[1], (SEQ, CELL_HEADS * HD), 1.0, 6.0, ((0, 8), (1, 4)))
    cell_value_heads = centred(arg_keys[2], (SEQ, CELL_HEADS * HD), 1.0, 6.0, ((0, 8), (1, 4)))
    output_gate_logits = centred(arg_keys[3], (SEQ, CELL_HEADS * HD), 1.0, 6.0, ((0, 8), (1, 4)))
    input_gate_log = draw_input_gate_log(jax.random.fold_in(arg_keys[17], 71), 0)
    forget_gate_logits = draw_forget_gate_logits(jax.random.fold_in(arg_keys[17], 71), 0)
    extra_log_decay = draw_extra_log_decay(jax.random.fold_in(arg_keys[17], 71), 0)
    documents = jnp.searchsorted(jnp.cumsum(ragged(arg_keys[7], DOCS, SEQ, DOC_MOST, 1)), jnp.arange(SEQ), side="right").astype(jnp.int32)
    head_norm_gain = jnp.clip(1.0 + 0.18 * jax.random.normal(arg_keys[8], (CELL_HEADS * HD,), jnp.float32), 0.1, 1.9)
    stream = centred(arg_keys[9], (SEQ, D), 1.0, 6.0, ((0, 8), (1, 4)))
    output_weight = centred(arg_keys[10], (CELL_HEADS * HD, D), (CELL_HEADS * HD) ** -0.5, 0.125, ((1, 4),))
    expert_norm_gain = jnp.clip(1.0 + 0.18 * jax.random.normal(arg_keys[11], (D,), jnp.float32), 0.099609375, 1.8984375).astype(jnp.bfloat16)
    expert_choice_index_keys = jax.random.split(jax.random.fold_in(arg_keys[12], 1), SEQ // TOKENS_PER_SHARD)
    expert_choice_index_turns = jax.random.permutation(jax.random.fold_in(arg_keys[12], 3), SEQ // TOKENS_PER_SHARD)
    expert_choice_index = jax.vmap(lambda own, number: assign_block(jax.random.fold_in(arg_keys[12], 2), own, number, TOKENS_PER_SHARD, EXPERTS, TOPK, CAP, 2))(expert_choice_index_keys, expert_choice_index_turns).reshape((SEQ, TOPK))
    routing_weight = jnp.clip(0.2 + 0.8 * jax.random.uniform(arg_keys[13], (SEQ, TOPK), jnp.float32) ** shard_levels(arg_keys[13], (SEQ, TOPK), ((0, 8),), -0.2, 0.2), 0.2, 1.0)
    gate_weight = centred(arg_keys[14], (EXPERTS, D, FF), D ** -0.5, 0.09375, ((0, 8), (2, 4)))
    up_weight = centred(arg_keys[15], (EXPERTS, D, FF), D ** -0.5, 0.09375, ((0, 8), (2, 4)))
    down_weight = centred(arg_keys[16], (EXPERTS, FF, D), FF ** -0.5, 0.125, ((0, 8), (2, 4)))
    return dict(cell_query_heads=cell_query_heads, cell_key_heads=cell_key_heads, cell_value_heads=cell_value_heads, output_gate_logits=output_gate_logits, input_gate_log=input_gate_log, forget_gate_logits=forget_gate_logits, extra_log_decay=extra_log_decay, documents=documents, head_norm_gain=head_norm_gain, stream=stream, output_weight=output_weight, expert_norm_gain=expert_norm_gain, expert_choice_index=expert_choice_index, routing_weight=routing_weight, gate_weight=gate_weight, up_weight=up_weight, down_weight=down_weight)


EPSILON = 1e-06
LOW_LOG = -1e+30
HIGHEST = lax.Precision.HIGHEST

def empty_summary(heads, width):
    return (jnp.zeros((heads, width, width), jnp.float32), jnp.zeros((heads, width), jnp.float32), jnp.full((heads,), LOW_LOG, jnp.float32), jnp.zeros((heads,), jnp.float32), jnp.zeros((), jnp.int32), jnp.full((), -1, jnp.int32), jnp.full((), -1, jnp.int32))

def block_summary(key_f, value_f, decay_logarithm, input_gate_log, documents, first_global):
    length = documents.shape[0]
    positions = jnp.arange(length, dtype=jnp.int32)
    cumulative = jnp.cumsum(decay_logarithm, axis=0)
    total_log = cumulative[-1]
    prior_log = cumulative - decay_logarithm
    starts = jnp.concatenate([jnp.reshape(first_global, (1,)), documents[1:] != documents[:-1]])
    inside = jnp.any(starts)
    last_start = jnp.max(jnp.where(starts, positions, -1))
    base_log = lax.optimization_barrier(jnp.sum(jnp.where((positions == last_start)[:, None], prior_log, 0.0), axis=0))
    in_last = (documents == documents[-1])[:, None]
    weight_log = total_log[None, :] - cumulative + input_gate_log
    peak_log = lax.optimization_barrier(jnp.max(jnp.where(in_last, weight_log, LOW_LOG), axis=0))
    peak_log = jnp.where(inside, jnp.maximum(peak_log, total_log - base_log), peak_log)
    weights = jnp.where(in_last, jnp.exp(jnp.minimum(weight_log - peak_log[None, :], 0.0)), 0.0)
    matrix = jnp.einsum('lhd,lhe->hde', weights[:, :, None] * key_f, value_f, precision=HIGHEST)
    normer = lax.optimization_barrier(jnp.sum(weights[:, :, None] * key_f, axis=0))
    return (matrix, normer, peak_log, total_log, inside.astype(jnp.int32), documents[0], documents[-1])

def combine(early, late):
    broken = late[5] != early[6]
    carry_matrix = jnp.where(broken, 0.0, early[0])
    carry_normer = jnp.where(broken, 0.0, early[1])
    carry_peak = jnp.where(broken, 0.0, early[2])
    joined = jnp.maximum(late[3] + carry_peak, late[2])
    older = jnp.exp(late[3] + carry_peak - joined)
    newer = jnp.exp(late[2] - joined)
    resets = late[4] > 0
    matrix = jnp.where(resets, late[0], older[:, None, None] * carry_matrix + newer[:, None, None] * late[0])
    normer = jnp.where(resets, late[1], older[:, None] * carry_normer + newer[:, None] * late[1])
    peak_log = jnp.where(resets, late[2], joined)
    flags = jnp.maximum(jnp.maximum(early[4], late[4]), broken.astype(jnp.int32))
    merged = (matrix, normer, peak_log, early[3] + late[3], flags, early[5], late[6])
    early_empty = early[6] < 0
    late_empty = late[6] < 0
    return tuple((jnp.where(early_empty, second, jnp.where(late_empty, first_item, joint)) for first_item, second, joint in zip(early, late, merged)))

def block_output(query_f, key_f, value_f, decay_logarithm, input_gate_log, documents, prefix):
    prev_matrix, prev_normer, prev_peak, _, _, _, prev_last = prefix
    length = documents.shape[0]
    positions = jnp.arange(length, dtype=jnp.int32)
    cumulative = jnp.cumsum(decay_logarithm, axis=0)
    prior_log = cumulative - decay_logarithm
    before = jnp.concatenate([jnp.reshape(prev_last, (1,)), documents[:-1]])
    starts = documents != before
    last_start = lax.cummax(jnp.where(starts, positions, -1), axis=0)
    started = last_start >= 0
    picker = (positions[None, :] == last_start[:, None]).astype(jnp.float32)
    base_log = jnp.dot(picker, prior_log, precision=HIGHEST)
    carry_log = (cumulative + jnp.where(started[:, None], -base_log, prev_peak[None, :])).T
    same_doc = (documents[:, None] == documents[None, :]) & (positions[:, None] >= positions[None, :])
    cum_heads = cumulative.T
    pair_log = cum_heads[:, :, None] - cum_heads[:, None, :] + input_gate_log.T[:, None, :]
    pair_log = jnp.where(same_doc[None], pair_log, LOW_LOG)
    peak_log = jnp.maximum(carry_log, lax.optimization_barrier(jnp.max(pair_log, axis=-1)))
    weights = jnp.exp(pair_log - peak_log[:, :, None])
    scores = jnp.einsum('lhd,shd->hls', query_f, key_f, precision=HIGHEST) * weights
    carry_scale = jnp.where(started[None, :], 0.0, jnp.exp(carry_log - peak_log))
    numer = jnp.einsum('hls,she->hle', scores, value_f, precision=HIGHEST)
    numer = numer + carry_scale[:, :, None] * jnp.einsum('lhd,hde->hle', query_f, prev_matrix, precision=HIGHEST)
    denom = lax.optimization_barrier(jnp.sum(scores, axis=-1)) + carry_scale * jnp.einsum('lhd,hd->hl', query_f, prev_normer, precision=HIGHEST)
    cell_vals = numer / jnp.maximum(jnp.abs(denom), jnp.exp(-peak_log))[:, :, None]
    return jnp.transpose(cell_vals, (1, 0, 2))

def finish_cell(cell_vals, output_gate_logits, head_norm_gain):
    length, heads, width = cell_vals.shape
    gated_cell = jax.nn.sigmoid(output_gate_logits.astype(jnp.float32)).reshape(length, heads, width) * cell_vals
    scaled = gated_cell * lax.rsqrt(lax.optimization_barrier(jnp.mean(gated_cell * gated_cell, axis=-1, keepdims=True)) + EPSILON)
    scaled = scaled * head_norm_gain.astype(jnp.float32).reshape(heads, width)
    return scaled.reshape(length, heads * width).astype(jnp.bfloat16)

def memory_cell_layer(cell_query_heads, cell_key_heads, cell_value_heads, output_gate_logits, input_gate_log, forget_gate_logits, extra_log_decay, documents, head_norm_gain):
    seq_len = documents.shape[0]
    block_list = seq_len // TOKENS_PER_SHARD
    shaped = (block_list, TOKENS_PER_SHARD, CELL_HEADS, HD)
    query_f = cell_query_heads.astype(jnp.float32).reshape(shaped)
    key_f = cell_key_heads.astype(jnp.float32).reshape(shaped) * HD ** (-0.5)
    value_f = cell_value_heads.astype(jnp.float32).reshape(shaped)
    decay_logarithm = (jax.nn.log_sigmoid(forget_gate_logits) + extra_log_decay).reshape(block_list, TOKENS_PER_SHARD, CELL_HEADS)
    gates = input_gate_log.reshape(block_list, TOKENS_PER_SHARD, CELL_HEADS)
    docs = documents.reshape(block_list, TOKENS_PER_SHARD)
    firsts = jnp.arange(block_list, dtype=jnp.int32) == 0
    summaries = lax.map(lambda items: block_summary(*items), (key_f, value_f, decay_logarithm, gates, docs, firsts))

    def advance(running, summary):
        return (combine(running, summary), running)
    _, prefixes = lax.scan(advance, empty_summary(CELL_HEADS, HD), summaries)
    cell_vals = lax.map(lambda items: block_output(*items), (query_f, key_f, value_f, decay_logarithm, gates, docs, prefixes))
    return finish_cell(cell_vals.reshape(seq_len, CELL_HEADS, HD), output_gate_logits, head_norm_gain)

def experts_layer(normed, expert_choice_index, routing_weight, gate_weight, up_weight, down_weight):
    seq_len = normed.shape[0]
    block_list = seq_len // TOKENS_PER_SHARD
    grouped = expert_choice_index.reshape(block_list, TOKENS_PER_SHARD * TOPK)
    onehot = (grouped[:, :, None] == jnp.arange(EXPERTS, dtype=jnp.int32)[None, None, :]).astype(jnp.int32)
    rank_in = lax.optimization_barrier(jnp.sum((jnp.cumsum(onehot, axis=1) - onehot) * onehot, axis=2))
    block_of = jnp.arange(block_list, dtype=jnp.int32)[:, None]
    slot_of = (grouped * (N_SP * CAP) + block_of * CAP + rank_in).reshape(-1).astype(jnp.int32)
    sources = jnp.repeat(normed, TOPK, axis=0)
    buffer = jnp.zeros((EXPERTS * N_SP * CAP, D), jnp.bfloat16).at[slot_of].set(sources)

    def run_expert(operands):
        row_block, gate_e, up_e, down_e = operands
        gate_act = jnp.dot(row_block, gate_e, preferred_element_type=jnp.float32)
        upward = jnp.dot(row_block, up_e, preferred_element_type=jnp.float32)
        hidden = (jax.nn.silu(gate_act) * upward).astype(jnp.bfloat16)
        return jnp.dot(hidden, down_e, preferred_element_type=jnp.float32).astype(jnp.bfloat16)
    served = lax.map(run_expert, (buffer.reshape(EXPERTS, N_SP * CAP, D), gate_weight, up_weight, down_weight))
    picked = served.reshape(-1, D)[slot_of].astype(jnp.float32).reshape(seq_len, TOPK, D)
    return lax.optimization_barrier(jnp.sum(picked * routing_weight[:, :, None], axis=1))

def reference(cell_query_heads, cell_key_heads, cell_value_heads, output_gate_logits, input_gate_log, forget_gate_logits, extra_log_decay, documents, head_norm_gain, stream, output_weight, expert_norm_gain, expert_choice_index, routing_weight, gate_weight, up_weight, down_weight):
    memory_cell_output = memory_cell_layer(cell_query_heads, cell_key_heads, cell_value_heads, output_gate_logits, input_gate_log, forget_gate_logits, extra_log_decay, documents, head_norm_gain)
    resid = (stream.astype(jnp.float32) + jnp.dot(memory_cell_output, output_weight, preferred_element_type=jnp.float32)).astype(jnp.bfloat16)
    rows_f = resid.astype(jnp.float32)
    normed = rows_f * lax.rsqrt(lax.optimization_barrier(jnp.mean(rows_f * rows_f, axis=1, keepdims=True)) + EPSILON)
    normed = (normed * expert_norm_gain.astype(jnp.float32)[None, :]).astype(jnp.bfloat16)
    mixed = experts_layer(normed, expert_choice_index, routing_weight, gate_weight, up_weight, down_weight)
    return (rows_f + mixed).astype(jnp.bfloat16)
```

```python
import functools

import jax
import jax.numpy as jnp
from jax import lax
from jax.experimental import pallas as pl
from jax.experimental.pallas import tpu as pltpu
from jax.sharding import PartitionSpec as P

HD = 128
TOPK = 2
EPSILON = 1e-06
LOW_LOG = -1e30
HIGHEST = lax.Precision.HIGHEST
GROUPS = 4


def swap(a, axis, mask):
    n = lax.axis_size(axis)
    return lax.ppermute(a, axis, [(i, i ^ mask) for i in range(n)])


def shift(a, axis, step):
    n = lax.axis_size(axis)
    return lax.ppermute(a, axis, [(i, i + step) for i in range(n - step)])


def nt_dot(a, b, **kw):
    return lax.dot_general(
        a, b, (((1,), (1,)), ((), ())), preferred_element_type=jnp.float32, **kw
    )


def cell_kernel(blocks, heads, *refs):
    query_ref, gate_ref, gain_ref = refs[:3]
    key_refs = refs[3 : 3 + blocks]
    value_refs = refs[3 + blocks : 3 + 2 * blocks]
    small_refs = refs[3 + 2 * blocks : 3 + 3 * blocks]
    out_ref = refs[-1]
    length = query_ref.shape[0]
    row = lax.broadcasted_iota(jnp.int32, (length, length), 0)
    col = lax.broadcasted_iota(jnp.int32, (length, length), 1)
    upper = (row <= col).astype(jnp.float32)
    eye = (row == col).astype(jnp.float32)
    offset = jnp.zeros((heads, 1), jnp.float32)
    cum, prior, lift, docs = [], [], [], []
    for b in range(blocks):
        small = small_refs[b][...]
        decay = small[0:heads]
        local = jnp.dot(small, upper, preferred_element_type=jnp.float32, precision=HIGHEST)
        total = local[0:heads] + offset
        cum.append(total)
        prior.append(total - decay)
        lift.append(small[heads : 2 * heads] - total)
        docs.append(small[2 * heads : 2 * heads + 1])
        offset = total[:, length - 1 : length]
    own = jnp.concatenate(
        [cum[-1], jnp.broadcast_to(docs[-1], (8, length))]
        + ([jnp.zeros((8 - heads, length), jnp.float32)] if heads < 8 else []),
        axis=0,
    )
    columns = nt_dot(eye, own, precision=HIGHEST)
    own_doc = columns[:, heads : heads + 1]
    masks = []
    for b in range(blocks):
        same = own_doc == docs[b]
        masks.append(same & (col <= row) if b == blocks - 1 else same)
    for h in range(heads):
        here = slice(h * HD, (h + 1) * HD)
        at = columns[:, h : h + 1]
        pair = []
        peak = jnp.full((length, 1), LOW_LOG, jnp.float32)
        whole = jnp.full((length, 1), -LOW_LOG, jnp.float32)
        for b in range(blocks):
            logs = jnp.where(masks[b], at + lift[b][h : h + 1], LOW_LOG)
            pair.append(logs)
            peak = jnp.maximum(peak, jnp.max(logs, axis=1, keepdims=True))
            span = jnp.where(masks[b], at - prior[b][h : h + 1], -LOW_LOG)
            whole = jnp.minimum(whole, jnp.min(span, axis=1, keepdims=True))
        stab = jnp.maximum(peak, whole)
        query = query_ref[:, here]
        numer = jnp.zeros((length, HD), jnp.float32)
        denom = jnp.zeros((length, 1), jnp.float32)
        for b in range(blocks):
            scores = nt_dot(query, key_refs[b][:, here]) * (HD ** (-0.5))
            scores = scores * jnp.exp(pair[b] - stab)
            denom = denom + jnp.sum(scores, axis=1, keepdims=True)
            high = scores.astype(jnp.bfloat16)
            low = (scores - high.astype(jnp.float32)).astype(jnp.bfloat16)
            value = value_refs[b][:, here]
            numer = numer + jnp.dot(high, value, preferred_element_type=jnp.float32)
            numer = numer + jnp.dot(low, value, preferred_element_type=jnp.float32)
        cell = numer / jnp.maximum(jnp.abs(denom), jnp.exp(-stab))
        gated = jax.nn.sigmoid(gate_ref[:, here].astype(jnp.float32)) * cell
        scale = lax.rsqrt(jnp.mean(gated * gated, axis=1, keepdims=True) + EPSILON)
        out_ref[:, here] = (gated * scale * gain_ref[:, here]).astype(jnp.bfloat16)


def run_cell(query, gates, gain, keys, values, smalls):
    blocks, heads = len(keys), query.shape[1] // HD
    return pl.pallas_call(
        functools.partial(cell_kernel, blocks, heads),
        out_shape=jax.ShapeDtypeStruct(query.shape, jnp.bfloat16),
        name="cell",
        cost_estimate=pl.CostEstimate(
            flops=12 * blocks * query.shape[0] * query.size,
            bytes_accessed=(4 + 2 * blocks) * query.size,
            transcendentals=0,
        ),
    )(query, gates, gain[None, :], *keys, *values, *smalls)


def tp_exchange(piece):
    n = lax.axis_size("tp")
    if n != 4:
        return [piece] + [swap(piece, "tp", m) for m in range(1, n)]
    half = piece.shape[0] // 2
    along_x, along_y = swap(piece, "tp", 1), swap(piece, "tp", 2)
    top = swap(along_y[:half], "tp", 1)
    bottom = swap(along_x[half:], "tp", 2)
    return [piece, along_x, along_y, jnp.concatenate([top, bottom], axis=0)]


def in_order(pieces):
    n, mine = len(pieces), lax.axis_index("tp")
    rows, width = pieces[0].shape
    whole = jnp.zeros((rows, n * width), pieces[0].dtype)
    for m, piece in enumerate(pieces):
        whole = lax.dynamic_update_slice(whole, piece, (0, jnp.bitwise_xor(mine, m) * width))
    return whole


def per_device(
    cell_query_heads,
    cell_key_heads,
    cell_value_heads,
    output_gate_logits,
    input_gate_log,
    forget_gate_logits,
    extra_log_decay,
    documents,
    head_norm_gain,
    stream,
    output_weight,
    expert_norm_gain,
    expert_choice_index,
    routing_weight,
    gate_weight,
    up_weight,
    down_weight,
):
    tokens = documents.shape[0]
    heads = input_gate_log.shape[1]
    sp, tp = lax.axis_size("sp"), lax.axis_size("tp")
    mine = lax.axis_index("sp")
    width = output_weight.shape[1] * tp
    back = (sp * tokens // 4 + tokens - 2) // tokens

    decay = jax.nn.log_sigmoid(forget_gate_logits) + extra_log_decay
    fill = (-(2 * heads + 1)) % 8
    small = jnp.concatenate(
        [
            decay.T,
            input_gate_log.T,
            (documents + 1).astype(jnp.float32)[None, :],
            jnp.zeros((fill, tokens), jnp.float32),
        ],
        axis=0,
    )
    keys, values, smalls = [cell_key_heads], [cell_value_heads], [small]
    for step in range(1, back + 1):
        keys.insert(0, shift(cell_key_heads, "sp", step))
        values.insert(0, shift(cell_value_heads, "sp", step))
        smalls.insert(0, shift(small, "sp", step))
    gain_all = in_order(
        [expert_norm_gain[None, :]]
        + [swap(expert_norm_gain[None, :], "tp", m) for m in range(1, tp)]
    )

    local_experts = gate_weight.shape[0]
    experts = sp * local_experts
    capacity = 2 * tokens * TOPK // experts
    slots = experts * capacity
    flat = expert_choice_index.reshape(-1)
    onehot = (flat[:, None] == jnp.arange(experts, dtype=jnp.int32)[None, :]).astype(jnp.bfloat16)
    places = jnp.arange(tokens * TOPK, dtype=jnp.int32)
    earlier = (places[:, None] > places[None, :]).astype(jnp.bfloat16)
    ahead = jnp.dot(earlier, onehot, preferred_element_type=jnp.float32)
    rank = jnp.sum(ahead * onehot.astype(jnp.float32), axis=1).astype(jnp.int32)
    there = jnp.bitwise_xor(flat // local_experts, mine) * local_experts + flat % local_experts
    slot_of = (there * capacity + rank).reshape(tokens, TOPK)
    slot_index = jnp.arange(slots, dtype=jnp.int32)
    chooser = jnp.any(slot_index[:, None, None] == slot_of[None, :, :], axis=2).astype(jnp.bfloat16)
    mixer = jnp.sum(
        jnp.where(slot_of[:, :, None] == slot_index[None, None, :], routing_weight[:, :, None], 0.0),
        axis=1,
    )
    mix_high = mixer.astype(jnp.bfloat16)
    mix_low = (mixer - mix_high.astype(jnp.float32)).astype(jnp.bfloat16)

    cell_out = run_cell(
        cell_query_heads, output_gate_logits, head_norm_gain, keys, values, smalls
    )
    cell_all = in_order([cell_out] + [swap(cell_out, "tp", m) for m in range(1, tp)])
    projected = jnp.dot(cell_all, output_weight, preferred_element_type=jnp.float32)
    resid = (stream.astype(jnp.float32) + projected).astype(jnp.bfloat16)
    packed = jnp.dot(chooser, resid, preferred_element_type=jnp.float32).astype(jnp.bfloat16)
    packed = packed.reshape(sp, local_experts * capacity, -1)

    rows = local_experts * capacity
    each = max(1, sp // GROUPS)
    mixed = resid.astype(jnp.float32)
    for start in range(0, sp, each):
        ks = list(range(start, min(sp, start + each)))
        arrived = [packed[k] if k == 0 else swap(packed[k], "sp", k) for k in ks]
        piece = jnp.stack(arrived, axis=0).reshape(len(ks), local_experts, capacity, -1)
        piece = jnp.swapaxes(piece, 0, 1).reshape(local_experts * len(ks) * capacity, -1)
        full = in_order(tp_exchange(piece))
        full_f = full.astype(jnp.float32)
        scale = lax.rsqrt(jnp.sum(full_f * full_f, axis=1, keepdims=True) / width + EPSILON)
        gained = (full_f * gain_all.astype(jnp.float32)).astype(jnp.bfloat16)
        gained = gained.reshape(local_experts, len(ks) * capacity, width)
        scale = scale.reshape(local_experts, len(ks) * capacity, 1)
        gate = jnp.einsum("qid,qdf->qif", gained, gate_weight, preferred_element_type=jnp.float32)
        up = jnp.einsum("qid,qdf->qif", gained, up_weight, preferred_element_type=jnp.float32)
        hidden = (jax.nn.silu(gate * scale) * (up * scale)).astype(jnp.bfloat16)
        hidden = in_order(tp_exchange(hidden.reshape(-1, hidden.shape[2])))
        hidden = hidden.reshape(local_experts, len(ks) * capacity, -1)
        served = jnp.einsum(
            "qif,qfe->qie", hidden, down_weight, preferred_element_type=jnp.float32
        ).astype(jnp.bfloat16)
        served = jnp.swapaxes(served.reshape(local_experts, len(ks), capacity, -1), 0, 1)
        served = served.reshape(len(ks), rows, -1)
        back_rows = [served[i] if k == 0 else swap(served[i], "sp", k) for i, k in enumerate(ks)]
        returned = jnp.concatenate(back_rows, axis=0)
        here = slice(start * rows, (start + len(ks)) * rows)
        mixed = mixed + jnp.dot(mix_high[:, here], returned, preferred_element_type=jnp.float32)
        mixed = mixed + jnp.dot(mix_low[:, here], returned, preferred_element_type=jnp.float32)
    return mixed.astype(jnp.bfloat16)


def solution(mesh):
    both = P("sp", "tp")
    placed = (
        (both,) * 7
        + (P("sp"), P("tp"), both, P(None, "tp"), P("tp"), P("sp", None), P("sp", None))
        + (P("sp", None, "tp"),) * 3
    )
    return jax.shard_map(
        per_device, mesh=mesh, in_specs=placed, out_specs=both, check_vma=False
    )
```

```python
import functools

import jax
import jax.numpy as jnp
from jax import lax
from jax.experimental import pallas as pl
from jax.experimental.pallas import tpu as pltpu
from jax.sharding import PartitionSpec as P


HD = 128
TOPK = 2
EPSILON = 1e-06
LOW_LOG = -1e30
HIGHEST = lax.Precision.HIGHEST
GROUPS = 4
BF16, F32 = jnp.bfloat16, jnp.float32
FIELDS = 16
KERNEL_VMEM = 16 << 20


PLAN = ((0, 1), (4,), (5, 6), (2, 3), (7,))
ROUTE = "xyxyy"


def swap(a, axis, mask):
    n = lax.axis_size(axis)
    return lax.ppermute(a, axis, [(i, i ^ mask) for i in range(n)])


def shift(a, axis, step):
    n = lax.axis_size(axis)
    return lax.ppermute(a, axis, [(i, (i + step) % n) for i in range(n)])


def nt_dot(a, b, **kw):
    return lax.dot_general(
        a, b, (((1,), (1,)), ((), ())), preferred_element_type=F32, **kw
    )


def dot(a, b):
    return jnp.dot(a, b, preferred_element_type=F32)


def call(kernel, outs, operands, flops, scratch=(), place=pltpu.VMEM):
    nbytes = 2 * sum(a.size * a.dtype.itemsize for a in operands)
    if place is pltpu.HBM:
        operands = [pltpu.with_memory_space_constraint(a, place) for a in operands]
    return pl.pallas_call(
        kernel,
        out_shape=outs,
        in_specs=[
            pl.BlockSpec(memory_space=pltpu.SMEM if a.size == 1 else place)
            for a in operands
        ],
        out_specs=[pl.BlockSpec(memory_space=pltpu.VMEM)] * len(outs),
        scratch_shapes=list(scratch),
        cost_estimate=pl.CostEstimate(flops=flops, bytes_accessed=nbytes, transcendentals=0),
        compiler_params=pltpu.CompilerParams(vmem_limit_bytes=KERNEL_VMEM),
    )(*operands)


def load_kernel(count, *refs):
    sources, targets, sems = refs[:count], refs[count : 2 * count], refs[-1]
    copies = [
        pltpu.make_async_copy(source, target, sems.at[i])
        for i, (source, target) in enumerate(zip(sources, targets))
    ]
    for copy in copies:
        copy.start()
    for copy in copies:
        copy.wait()


def load(*arrays):
    return call(
        functools.partial(load_kernel, len(arrays)),
        [pltpu.VMEM(a.shape, a.dtype) for a in arrays],
        arrays,
        1,
        [pltpu.SemaphoreType.DMA((len(arrays),))],
        pltpu.HBM,
    )


def block_kernel(key_ref, value_ref, forget_ref, extra_ref, lift_ref, docs_ref, out_ref, *scratch):
    length, width = key_ref.shape
    forget, extra, lift, docs, sems = scratch
    moves = (
        (key_ref, out_ref.at[:, :width]),
        (value_ref, out_ref.at[:, width : 2 * width]),
        (forget_ref, forget),
        (extra_ref, extra),
        (lift_ref, lift),
        (docs_ref, docs),
    )
    copies = [
        pltpu.make_async_copy(source, target, sems.at[i])
        for i, (source, target) in enumerate(moves)
    ]
    for copy in copies:
        copy.start()
    for copy in copies[2:]:
        copy.wait()
    decay = jax.nn.log_sigmoid(forget[...]) + extra[...]
    heads = decay.shape[0]
    number = docs[...].astype(F32) + 1.0
    small = jnp.concatenate(
        [decay, lift[...], number, jnp.zeros((FIELDS - 2 * heads - 1, length), F32)], axis=0
    )
    parts = split3(small)
    parts.append(jnp.zeros((length - 3 * FIELDS, length), BF16))
    out_ref[:, 2 * width :] = jnp.concatenate(parts, axis=0)
    for copy in copies[:2]:
        copy.wait()


def cat_kernel(first_ref, *refs):
    out_ref, rows = refs[-1], first_ref.shape[0]
    for i, ref in enumerate((first_ref, *refs[:-1])):
        out_ref[i * rows : (i + 1) * rows, :] = ref[...]


def split3(a):
    high = a.astype(BF16)
    rest = a - high.astype(F32)
    middle = rest.astype(BF16)
    return [high, middle, (rest - middle.astype(F32)).astype(BF16)]


def cell_kernel(blocks, heads, *refs):
    query_ref, gate_ref, gain_ref = refs[:3]
    block_refs = refs[3 : 3 + blocks]
    out_ref = refs[-1]
    length, width = query_ref.shape
    row = lax.broadcasted_iota(jnp.int32, (length, length), 0)
    col = lax.broadcasted_iota(jnp.int32, (length, length), 1)
    upper = (row <= col).astype(F32)
    eye = (row == col).astype(F32)
    offset = jnp.zeros((heads, 1), F32)
    cum, prior, lift, docs = [], [], [], []
    for b in range(blocks):
        small = sum(
            block_refs[b][i * FIELDS : (i + 1) * FIELDS, 2 * width :].astype(F32) for i in range(3)
        )
        decay = small[0:heads]
        local = jnp.dot(small, upper, preferred_element_type=F32, precision=HIGHEST)
        total = local[0:heads] + offset
        cum.append(total)
        prior.append(total - decay)
        lift.append(small[heads : 2 * heads] - total)
        docs.append(small[2 * heads : 2 * heads + 1])
        offset = total[:, length - 1 : length]
    own = jnp.concatenate(
        [cum[-1], jnp.broadcast_to(docs[-1], (8, length))]
        + ([jnp.zeros((8 - heads, length), F32)] if heads < 8 else []),
        axis=0,
    )
    columns = nt_dot(eye, own, precision=HIGHEST)
    own_doc = columns[:, heads : heads + 1]
    masks = []
    for b in range(blocks):
        same = own_doc == docs[b]
        masks.append(same & (col <= row) if b == blocks - 1 else same)
    for h in range(heads):
        here = slice(h * HD, (h + 1) * HD)
        at = columns[:, h : h + 1]
        pair, peak, whole = [], None, None
        for b in range(blocks):
            logs = jnp.where(masks[b], at + lift[b][h : h + 1], LOW_LOG)
            pair.append(logs)
            peak = logs if b == 0 else jnp.maximum(peak, logs)
            span = jnp.where(masks[b], at - prior[b][h : h + 1], -LOW_LOG)
            whole = span if b == 0 else jnp.minimum(whole, span)
        peak = jnp.max(peak, axis=1, keepdims=True)
        stab = jnp.maximum(peak, jnp.min(whole, axis=1, keepdims=True))
        query = query_ref[:, here]
        numer, denom = None, None
        for b in range(blocks):
            scores = nt_dot(query, block_refs[b][:, here]) * (HD ** (-0.5))
            scores = scores * jnp.exp(pair[b] - stab)
            denom = scores if b == 0 else denom + scores
            high = scores.astype(BF16)
            low = (scores - high.astype(F32)).astype(BF16)
            value = block_refs[b][:, width + h * HD : width + (h + 1) * HD]
            part = dot(high, value) + dot(low, value)
            numer = part if b == 0 else numer + part
        denom = jnp.sum(denom, axis=1, keepdims=True)
        cell = numer / jnp.maximum(jnp.abs(denom), jnp.exp(-stab))
        gated = jax.nn.sigmoid(gate_ref[:, here].astype(F32)) * cell
        scale = lax.rsqrt(jnp.mean(gated * gated, axis=1, keepdims=True) + EPSILON)
        out_ref[:, here] = (gated * scale * gain_ref[:, here]).astype(BF16)


def owned(pos_ref, member, size):
    at = jnp.bitwise_xor(pos_ref[0], member) * size
    return pl.ds(pl.multiple_of(at, size), size)


def pack_kernel(tp, pos_ref, stream_ref, chooser_ref, weight_ref, *refs):
    pieces, (resid_ref, *packed_refs) = refs[:tp], refs[tp:]
    total = stream_ref[...].astype(F32)
    for m, piece in enumerate(pieces):
        total = total + dot(piece[...], weight_ref[owned(pos_ref, m, piece.shape[1]), :])
    resid = total.astype(BF16)
    resid_ref[...] = resid
    rows = packed_refs[0].shape[0]
    for k, packed in enumerate(packed_refs):
        packed[...] = dot(chooser_ref[k * rows : (k + 1) * rows, :], resid).astype(BF16)


def up_kernel(tp, pos_ref, gain_ref, gate_ref, up_ref, *refs):
    pieces, hidden_ref, (gate_acc, up_acc) = refs[:tp], refs[tp], refs[tp + 1 :]
    rows, width = pieces[0].shape
    squares = jnp.zeros((rows, 1), F32)
    for m, piece in enumerate(pieces):
        here = owned(pos_ref, m, width)
        full = piece[...].astype(F32)
        squares = squares + jnp.sum(full * full, axis=1, keepdims=True)
        gain = gain_ref[m : m + 1, :].astype(F32)
        gained = (full * gain).astype(BF16)
        for acc, weight in ((gate_acc, gate_ref), (up_acc, up_ref)):
            part = dot(gained, weight[here, :])
            acc[...] = part if m == 0 else acc[...] + part
    scale = lax.rsqrt(squares / (tp * width) + EPSILON)
    hidden_ref[...] = (jax.nn.silu(gate_acc[...] * scale) * (up_acc[...] * scale)).astype(BF16)


def down_kernel(tp, pos_ref, weight_ref, *refs):
    pieces, out_refs = refs[:tp], refs[tp:]
    total = None
    for m, piece in enumerate(pieces):
        part = dot(piece[...], weight_ref[owned(pos_ref, m, piece.shape[1]), :])
        total = part if m == 0 else total + part
    rows = out_refs[0].shape[0]
    for i, out in enumerate(out_refs):
        out[...] = total[i * rows : (i + 1) * rows].astype(BF16)


def mix_kernel(resid_ref, high_ref, low_ref, *refs):
    pieces, out_ref, all_ref = refs[:-2], refs[-2], refs[-1]
    rows = pieces[0].shape[0]
    for k, piece in enumerate(pieces):
        all_ref[k * rows : (k + 1) * rows, :] = piece[...]
    total = resid_ref[...].astype(F32) + dot(high_ref[...], all_ref[...])
    out_ref[...] = (total + dot(low_ref[...], all_ref[...])).astype(BF16)


def tp_exchange(piece, last_axis):
    n = lax.axis_size("tp")
    if n != 4:
        return [piece] + [swap(piece, "tp", m) for m in range(1, n)]
    along_x = swap(piece, "tp", 1)
    along_y = swap(piece, "tp", 2)
    if last_axis == "y":
        diagonal = swap(along_x, "tp", 2)
    else:
        diagonal = swap(along_y, "tp", 1)
    return [piece, along_x, along_y, diagonal]


def per_device(
    cell_query_heads,
    cell_key_heads,
    cell_value_heads,
    output_gate_logits,
    input_gate_log,
    forget_gate_logits,
    extra_log_decay,
    documents,
    head_norm_gain,
    stream,
    output_weight,
    expert_norm_gain,
    expert_choice_index,
    routing_weight,
    gate_weight,
    up_weight,
    down_weight,
):
    tokens = documents.shape[0]
    heads = input_gate_log.shape[1]
    sp, tp = lax.axis_size("sp"), lax.axis_size("tp")
    mine = lax.axis_index("sp")
    pos = lax.axis_index("tp").astype(jnp.int32).reshape(1)
    back = (sp * tokens // 4 + tokens - 2) // tokens

    width = cell_key_heads.shape[1]
    (block,) = call(
        block_kernel,
        [jax.ShapeDtypeStruct((tokens, 2 * width + tokens), BF16)],
        [
            cell_key_heads,
            cell_value_heads,
            forget_gate_logits.T,
            extra_log_decay.T,
            input_gate_log.T,
            documents[None, :],
        ],
        1,
        [pltpu.VMEM((heads, tokens), F32)] * 3
        + [pltpu.VMEM((1, tokens), jnp.int32), pltpu.SemaphoreType.DMA((6,))],
        pltpu.HBM,
    )
    blocks = [block]
    for step in range(1, back + 1):
        blocks.insert(0, shift(block, "sp", step))
    gains = [expert_norm_gain[None, :]]
    gains += [swap(gains[0], "tp", m) for m in range(1, tp)]
    gain_all = jnp.concatenate(gains, axis=0)

    local_experts = gate_weight.shape[0]
    assert local_experts == 1
    experts = sp * local_experts
    capacity = 2 * tokens * TOPK // experts
    slots = experts * capacity
    flat = expert_choice_index.reshape(-1)
    onehot = (flat[:, None] == jnp.arange(experts, dtype=jnp.int32)[None, :]).astype(BF16)
    places = jnp.arange(tokens * TOPK, dtype=jnp.int32)
    earlier = (places[:, None] > places[None, :]).astype(BF16)
    ahead = dot(earlier, onehot)
    rank = jnp.sum(ahead * onehot.astype(F32), axis=1).astype(jnp.int32)
    slot_of = (jnp.bitwise_xor(flat, mine) * capacity + rank).reshape(tokens, TOPK)
    slot_index = jnp.arange(slots, dtype=jnp.int32)
    chooser = jnp.any(slot_index[:, None, None] == slot_of[None, :, :], axis=2).astype(BF16)
    mixer = jnp.sum(
        jnp.where(slot_of[:, :, None] == slot_index[None, None, :], routing_weight[:, :, None], 0.0),
        axis=1,
    )
    mix_high = mixer.astype(BF16)
    mix_low = (mixer - mix_high.astype(F32)).astype(BF16)

    def like(rows, columns):
        return jax.ShapeDtypeStruct((rows, columns), BF16)

    query, out_gate, head_gain = load(cell_query_heads, output_gate_logits, head_norm_gain[None, :])
    (cell_out,) = call(
        functools.partial(cell_kernel, len(blocks), heads),
        [like(*cell_query_heads.shape)],
        [query, out_gate, head_gain, *blocks],
        12 * len(blocks) * tokens * cell_query_heads.size,
    )
    cells = [cell_out] + [swap(cell_out, "tp", m) for m in range(1, tp)]
    features = stream.shape[1]
    stream_v, out_weight = load(stream, output_weight)
    gate_v, up_v, down_v = load(gate_weight[0], up_weight[0], down_weight[0])
    resid, *packed = call(
        functools.partial(pack_kernel, tp),
        [like(tokens, features)] + [like(capacity, features)] * sp,
        [pos, stream_v, chooser, out_weight, *cells],
        2 * tokens * output_weight.size + 2 * slots * tokens * features,
    )
    each = sp // GROUPS
    near = [range(i * each, (i + 1) * each) for i in range(GROUPS)]
    plan = PLAN if planned(sp, tp) else (near[0], *near[2:], near[1])
    results = [None] * sp
    for group, ks in enumerate(plan):
        arrived = [packed[k] if k == 0 else swap(packed[k], "sp", k) for k in ks]
        rows = len(ks) * capacity
        piece = arrived[0]
        if len(arrived) > 1:
            (piece,) = call(cat_kernel, [like(rows, features)], arrived, 1)
        last_axis = ROUTE[group % len(ROUTE)]
        pieces = tp_exchange(piece, last_axis)
        (hidden,) = call(
            functools.partial(up_kernel, tp),
            [like(rows, gate_v.shape[1])],
            [pos, gain_all, gate_v, up_v, *pieces],
            4 * rows * gate_v.size,
            [pltpu.VMEM((rows, gate_v.shape[1]), F32)] * 2,
        )
        hiddens = tp_exchange(hidden, last_axis)
        served = call(
            functools.partial(down_kernel, tp),
            [like(capacity, features)] * len(ks),
            [pos, down_v, *hiddens],
            2 * rows * down_v.size,
        )
        for k, result in zip(ks, served):
            results[k] = result if k == 0 else swap(result, "sp", k)
    (out,) = call(
        mix_kernel,
        [like(tokens, features)],
        [resid, mix_high, mix_low, *results],
        4 * tokens * slots * features,
        [pltpu.VMEM((slots, features), BF16)],
    )
    return out


def planned(sp, tp):
    return tp == 4 and sorted(k for ks in PLAN for k in ks) == list(range(sp))


def solution(mesh):
    both = P("sp", "tp")
    placed = (
        (both,) * 7
        + (P("sp"), P("tp"), both, P(None, "tp"), P("tp"), P("sp", None), P("sp", None))
        + (P("sp", None, "tp"),) * 3
    )

    return jax.shard_map(per_device, mesh=mesh, in_specs=placed, out_specs=both, check_vma=False)
```
